512 devices in a mesh: grp: 2 (over y), tp: 32 (over z), dp: 8 (over x, core).
Axes of the slice: x: 4, y: 2, z: 32, core: 2. Of those that a mesh axis runs over, the one named last changes fastest.
The devices are a block of a 4x8x32 slice.
Arguments:
- hidden_in: bfloat16 [192, 4096], P(('grp', 'tp'), 'dp'), parts along dimension 0, may hold values from -40 to 40
- input_norm_gain: float32 [2, 4096], P(None, 'dp'), may hold values from 0.1 to 1.9
- w_query: bfloat16 [2, 4096, 2048], P(None, 'dp', 'tp'), may hold values from -0.09375 to 0.09375
- w_key: bfloat16 [2, 4096, 2048], P(None, 'dp', 'tp'), may hold values from -0.09375 to 0.09375
- w_decay: bfloat16 [2, 4096, 2048], P(None, 'dp', 'tp'), may hold values from -0.375 to 0.375
- w_value: bfloat16 [2, 4096, 4096], P(None, 'dp', 'tp'), may hold values from -0.09375 to 0.09375
- w_gate: bfloat16 [2, 4096, 4096], P(None, 'dp', 'tp'), may hold values from -0.09375 to 0.09375
- out_gain: float32 [2, 4096], P(None, 'tp'), may hold values from 0.1 to 1.9
- w_out: bfloat16 [2, 4096, 4096], P(None, 'tp', 'dp'), may hold values from -0.09375 to 0.09375
- decay_offset: float32 [2, 192, 2048], P(None, ('grp', 'dp'), 'tp'), parts along dimension 1, may hold values from -0.7 to 0
- state: float32 [2, 192, 32, 64, 128], P(None, ('grp', 'dp'), 'tp'), parts along dimension 1, may hold values from -3 to 3
Outputs:
- hidden_out: bfloat16 [192, 4096], P(('grp', 'tp'), 'dp'), parts along dimension 0
- new_state: float32 [2, 192, 32, 64, 128], P(None, ('grp', 'dp'), 'tp'), parts along dimension 1
The draws below stay inside these ranges and needn't reach their ends.
There are 2 independent parts, one for each index of `grp`. The reference program is written for one: setup_inputs(seed, part) draws one part's arguments, and reference() takes and returns one part's arrays. A program takes and returns all parts, laid end to end along the dimension named above; an argument that names none is the same for every part. Nothing has to cross between parts.
All inputs are finite; a program needn't handle non-finite values.
Results may differ from the reference program's by a relative error of at most 0.017.
Values may be sent and summed in bfloat16 or wider, within the bound.
No kernel may reach another device: no remote copies, remote signals or barrier semaphores. Data moves between devices by JAX's collectives and lax.ppermute only.
A program may use at most 64 MiB of HBM per device.

```python
import jax
import jax.numpy as jnp
from jax import lax

D = 4096
HEADS = 32
HEAD_KEY = 64
VALUE_CHANNELS = 128
LAYERS = 2
BATCH = 96
KEY_W = 2048
VAL_W = 4096
N_DP = 8


def draw_hidden_in(key, part):
    base_key, column_key, row_key = jax.random.split(key, 3)
    column = jnp.arange(D, dtype=jnp.float32) / (D - 1)
    column_scale = jnp.exp(jnp.log(3.0) * column + jax.random.uniform(column_key, (D,), jnp.float32, -0.5, 0.5))
    values = jnp.clip(jax.random.normal(base_key, (BATCH, D), jnp.float32), -4.0, 4.0)
    row_scale = jnp.exp(jax.random.uniform(row_key, (BATCH, 1), jnp.float32, -0.7, 0.7))
    return (values * row_scale * column_scale[None, :]).astype(jnp.bfloat16)


def level_of(own_key, extent, shards, low, largest):
    level = 1.0
    for position, blocks in shards:
        steps = jax.random.uniform(jax.random.fold_in(jax.random.fold_in(own_key, 6), position), (blocks,), jnp.float32, low / len(shards), largest / len(shards))
        level = level * jnp.repeat(jnp.exp(steps), extent[position] // blocks).reshape((-1,) + (1,) * (len(extent) - 1 - position))
    return level


def bell_draw(stream_key, dims, scale, bound, cuts=(), kind=jnp.bfloat16):
    result = scale * jax.random.normal(stream_key, dims, jnp.float32)
    if cuts:
        result = result * level_of(stream_key, dims, cuts, -0.22, 0.18)
    return jnp.clip(result, -bound, bound).astype(kind)


def setup_inputs(seed: int = 0, part: int = 0) -> dict:
    arg_keys = jax.random.split(jax.random.key(seed), 12)
    part_keys = jax.random.split(jax.random.fold_in(arg_keys[11], part), 12)
    hidden_in = draw_hidden_in(jax.random.fold_in(jax.random.fold_in(arg_keys[11], part), 71), part)
    input_norm_gain = jnp.clip(1.0 + 0.18 * jax.random.normal(arg_keys[1], (LAYERS, D), jnp.float32), 0.1, 1.9)
    w_query = bell_draw(arg_keys[2], (LAYERS, D, KEY_W), D ** -0.5, 0.09375, ((1, 8), (2, 32)))
    w_key = bell_draw(arg_keys[3], (LAYERS, D, KEY_W), D ** -0.5, 0.09375, ((1, 8), (2, 32)))
    w_decay = bell_draw(arg_keys[4], (LAYERS, D, KEY_W), (D // 16) ** -0.5, 0.375, ((1, 8), (2, 32)))
    w_value = bell_draw(arg_keys[5], (LAYERS, D, VAL_W), D ** -0.5, 0.09375, ((1, 8), (2, 32)))
    w_gate = bell_draw(arg_keys[6], (LAYERS, D, VAL_W), D ** -0.5, 0.09375, ((1, 8), (2, 32)))
    out_gain = jnp.clip(1.0 + 0.18 * jax.random.normal(arg_keys[7], (LAYERS, VAL_W), jnp.float32), 0.1, 1.9)
    w_out = bell_draw(arg_keys[8], (LAYERS, VAL_W, D), VAL_W ** -0.5, 0.09375, ((1, 32), (2, 8)))
    decay_offset = jnp.clip(-0.7 + 0.7 * jax.random.uniform(part_keys[9], (LAYERS, BATCH, KEY_W), jnp.float32) ** level_of(part_keys[9], (LAYERS, BATCH, KEY_W), ((1, 8), (2, 32)), -0.2, 0.2), -0.7, 0.0)
    state = bell_draw(part_keys[10], (LAYERS, BATCH, HEADS, HEAD_KEY, VALUE_CHANNELS), 0.5, 3.0, ((1, 8), (2, 32)), jnp.float32)
    return dict(hidden_in=hidden_in, input_norm_gain=input_norm_gain, w_query=w_query, w_key=w_key, w_decay=w_decay, w_value=w_value, w_gate=w_gate, out_gain=out_gain, w_out=w_out, decay_offset=decay_offset, state=state)


epsilon = 1e-06
softness_factor = 16.0

def reference(hidden_in, input_norm_gain, w_query, w_key, w_decay, w_value, w_gate, out_gain, w_out, decay_offset, state):
    hidden = hidden_in
    states = []
    for index_of_block in range(LAYERS):
        widened = hidden.astype(jnp.float32)
        squares = lax.optimization_barrier(jnp.sum(widened * widened, axis=1))
        scaled_query = (widened * input_norm_gain[index_of_block][None, :]).astype(jnp.bfloat16)
        groups = scaled_query.astype(jnp.float32).reshape(BATCH, N_DP, D // N_DP)
        pieces = []
        for matrix in (w_query, w_key, w_decay, w_value, w_gate):
            blocks = matrix[index_of_block].astype(jnp.float32).reshape(N_DP, D // N_DP, matrix.shape[2])
            partial_value = jnp.einsum('bnr,nrc->nbc', groups, blocks, precision=lax.Precision.HIGHEST)
            rounded = lax.optimization_barrier(partial_value.astype(jnp.bfloat16))
            pieces.append(lax.optimization_barrier(jnp.sum(rounded.astype(jnp.float32), axis=0)))
        inverse = lax.rsqrt(squares / D + epsilon)[:, None]
        query_rows = (pieces[0] * inverse).reshape(BATCH, HEADS, HEAD_KEY)
        key_rows = (pieces[1] * inverse).reshape(BATCH, HEADS, HEAD_KEY) * HEAD_KEY ** (-0.5)
        decay_logits = pieces[2] * inverse
        value_rows = (pieces[3] * inverse).reshape(BATCH, HEADS, VALUE_CHANNELS)
        gate_rows = (pieces[4] * inverse).reshape(BATCH, HEADS, VALUE_CHANNELS)
        decay_logarithm = jax.nn.log_sigmoid(decay_logits) / softness_factor + decay_offset[index_of_block]
        decay_rate = jnp.exp(decay_logarithm).reshape(BATCH, HEADS, HEAD_KEY)
        fresh = decay_rate[:, :, :, None] * state[index_of_block] + key_rows[:, :, :, None] * value_rows[:, :, None, :]
        readout = lax.optimization_barrier(jnp.sum(query_rows[:, :, :, None] * fresh, axis=2))
        normed = readout * lax.rsqrt(lax.optimization_barrier(jnp.mean(readout * readout, axis=2, keepdims=True)) + epsilon)
        normed = normed * out_gain[index_of_block].reshape(HEADS, VALUE_CHANNELS)[None]
        gated_out = (normed * jax.nn.silu(gate_rows)).reshape(BATCH, VAL_W).astype(jnp.bfloat16)
        mixed = jnp.dot(gated_out, w_out[index_of_block], preferred_element_type=jnp.float32)
        hidden = (widened + mixed).astype(jnp.bfloat16)
        states.append(fresh)
    return (hidden, jnp.stack(states))
```

```python
import jax
import jax.numpy as jnp
from jax import lax
from jax.sharding import Mesh, PartitionSpec as P

D = 4096
HEAD_KEY = 64
VALUE_CHANNELS = 128
LAYERS = 2
LANES = 128
NEAR = 4


epsilon = 1e-06
softness_factor = 16.0

TP = ("far", "near")


def size_of(axes):
    return lax.psum(1, axes)


def exchange(blocks, axes):
    return lax.all_to_all(blocks, axes, split_axis=0, concat_axis=0, tiled=True)


def copies(value, axes):
    return exchange(jnp.broadcast_to(value[None], (size_of(axes), *value.shape)), axes)


def summed(blocks):
    return blocks.astype(jnp.float32).sum(axis=0)


def two_terms(value):
    high = lax.reduce_precision(value, 8, 7)
    return high.astype(jnp.bfloat16), (value - high).astype(jnp.bfloat16)


def per_device(
    hidden_in,
    input_norm_gain,
    w_query,
    w_key,
    w_decay,
    w_value,
    w_gate,
    out_gain,
    w_out,
    decay_offset,
    state,
):
    seq_rows = state.shape[1]
    local_heads = state.shape[2]
    key_cols = local_heads * HEAD_KEY
    value_cols = local_heads * VALUE_CHANNELS
    own_rows, features = hidden_in.shape
    n_dp = size_of("dp")
    n_near = size_of("near")
    hidden = copies(hidden_in, TP).reshape(-1, features)
    own_hidden = hidden_in
    batch = hidden.shape[0]
    states = []
    for index_of_block in range(LAYERS):
        widened = hidden.astype(jnp.float32)
        squares = jnp.sum(widened * widened, axis=1, keepdims=True)
        scaled = (widened * input_norm_gain[index_of_block][None, :]).astype(jnp.bfloat16)
        partial_value = [
            jnp.dot(scaled, matrix[index_of_block], preferred_element_type=jnp.float32).astype(
                jnp.bfloat16
            )
            for matrix in (w_value, w_gate, w_query, w_key, w_decay)
        ]
        used = 2 * value_cols + 3 * key_cols
        spare = -(used + 2) % LANES
        sent = jnp.concatenate(
            [*partial_value, *two_terms(squares), jnp.zeros((batch, spare), jnp.bfloat16)], axis=1
        )
        summed_parts = summed(exchange(sent.reshape(n_dp, seq_rows, -1), "dp"))
        own_squares = jnp.sum(summed_parts[:, used : used + 2], axis=1, keepdims=True)
        inverse = lax.rsqrt(own_squares / D + epsilon)
        projected = summed_parts[:, :used] * inverse
        value_rows = projected[:, :value_cols].reshape(seq_rows, local_heads, VALUE_CHANNELS)
        gate_rows = projected[:, value_cols : 2 * value_cols].reshape(
            seq_rows, local_heads, VALUE_CHANNELS
        )
        rest = projected[:, 2 * value_cols :]
        query_rows = rest[:, :key_cols].reshape(seq_rows, local_heads, HEAD_KEY)
        key_rows = rest[:, key_cols : 2 * key_cols].reshape(
            seq_rows, local_heads, HEAD_KEY
        ) * HEAD_KEY ** (-0.5)
        decay_logits = rest[:, 2 * key_cols :]
        decay_logarithm = (
            jax.nn.log_sigmoid(decay_logits) / softness_factor + decay_offset[index_of_block]
        )
        decay_rate = jnp.exp(decay_logarithm).reshape(seq_rows, local_heads, HEAD_KEY)
        fresh = (
            decay_rate[:, :, :, None] * state[index_of_block]
            + key_rows[:, :, :, None] * value_rows[:, :, None, :]
        )
        states.append(fresh)
        readout = jnp.sum(query_rows[:, :, :, None] * fresh, axis=2)
        normed = readout * lax.rsqrt(jnp.mean(readout * readout, axis=2, keepdims=True) + epsilon)
        normed = normed * out_gain[index_of_block].reshape(local_heads, VALUE_CHANNELS)[None]
        gated_out = (
            (normed * jax.nn.silu(gate_rows)).reshape(seq_rows, value_cols).astype(jnp.bfloat16)
        )
        head_terms = jnp.dot(
            copies(gated_out, "dp").reshape(batch, value_cols),
            w_out[index_of_block],
            preferred_element_type=jnp.float32,
        ).astype(jnp.bfloat16)
        if index_of_block + 1 == LAYERS:
            own_part = summed(exchange(head_terms.reshape(-1, own_rows, features), TP))
            own_hidden = (own_hidden.astype(jnp.float32) + own_part).astype(jnp.bfloat16)
        else:
            near_sum = summed(exchange(head_terms.reshape(n_near, -1, features), "near"))
            far_sum = summed(copies(near_sum.astype(jnp.bfloat16), "far"))
            before = lax.dynamic_index_in_dim(
                hidden.reshape(n_near, -1, features), lax.axis_index("near"), 0, keepdims=False
            )
            after = (before.astype(jnp.float32) + far_sum).astype(jnp.bfloat16)
            hidden = copies(after, "near").reshape(batch, features)
            own_hidden = lax.dynamic_index_in_dim(
                hidden.reshape(-1, own_rows, features), lax.axis_index(TP), 0, keepdims=False
            )
    return (own_hidden, jnp.stack(states))


def solution(mesh):
    sizes = mesh.shape
    fine = Mesh(
        mesh.devices.reshape(sizes["grp"], sizes["tp"] // NEAR, NEAR, sizes["dp"]),
        ("grp", *TP, "dp"),
    )
    return jax.shard_map(
        per_device,
        mesh=fine,
        in_specs=(
            P(("grp", *TP), "dp"),
            P(None, "dp"),
            P(None, "dp", TP),
            P(None, "dp", TP),
            P(None, "dp", TP),
            P(None, "dp", TP),
            P(None, "dp", TP),
            P(None, TP),
            P(None, TP, "dp"),
            P(None, ("grp", "dp"), TP),
            P(None, ("grp", "dp"), TP, None, None),
        ),
        out_specs=(P(("grp", *TP), "dp"), P(None, ("grp", "dp"), TP, None, None)),
        check_vma=False,
    )
```

```python
import jax
import jax.numpy as jnp
from jax import lax
from jax.sharding import Mesh, PartitionSpec as P

D = 4096
HEAD_KEY = 64
VALUE_CHANNELS = 128
NEAR = 4
CORES = 2


epsilon = 1e-06
softness_factor = 16.0

TP = ("far", "near")
DP = ("x", "core")
LOCAL = ("near", *DP)


def size_of(axes):
    return lax.psum(1, axes)


def exchange(blocks, axes):
    return lax.all_to_all(blocks, axes, split_axis=0, concat_axis=0, tiled=True)


def copies(value, axes):
    return exchange(jnp.broadcast_to(value[None], (size_of(axes), *value.shape)), axes)


def summed(blocks):
    return blocks.astype(jnp.float32).sum(axis=0)


def dot(left, right):
    return jnp.dot(left, right, preferred_element_type=jnp.float32)


def from_ring(value):
    n = size_of("x")
    onward = [(i, (i + 1) % n) for i in range(n)]
    back = [(i, (i - 1) % n) for i in range(n)]
    half = value.shape[0] // 2
    found = {0: value}
    ahead = behind = value
    for step in range(1, n // 2 + 1):
        if 2 * step == n:
            ahead = lax.ppermute(ahead[:half], "x", onward)
            behind = lax.ppermute(behind[half:], "x", back)
            found[step] = jnp.concatenate([ahead, behind], axis=0)
        else:
            found[step] = ahead = lax.ppermute(ahead, "x", onward)
            found[n - step] = behind = lax.ppermute(behind, "x", back)
    return jnp.stack([found[i] for i in range(n)])


def from_all(value):
    ours = from_ring(value)
    return ours, lax.ppermute(ours, "core", [(0, 1), (1, 0)])


def turned(blocks):
    n, cores = size_of("x"), size_of("core")
    blocks = blocks.reshape(n, cores, *blocks.shape[1:])
    place = lax.axis_index("x")
    chips = [
        lax.dynamic_index_in_dim(blocks, lax.rem(place - s + n, n), 0, keepdims=False)
        for s in range(n)
    ]
    blocks = jnp.stack(chips, axis=1)
    return jnp.where(lax.axis_index("core") == 0, blocks, blocks[::-1])


def turned_back(blocks):
    n = size_of("x")
    place = lax.axis_index("x")
    blocks = jnp.where(lax.axis_index("core") == 0, blocks, blocks[::-1])
    chips = [
        lax.dynamic_index_in_dim(blocks, lax.rem(place - s + n, n), 1, keepdims=False)
        for s in range(n)
    ]
    blocks = jnp.stack(chips, axis=0)
    return blocks.reshape(-1, *blocks.shape[2:])


def three_terms(value):
    terms = []
    for _ in range(3):
        term = lax.reduce_precision(value, 8, 7)
        terms.append(term.astype(jnp.bfloat16))
        value = value - term
    return terms


def mixed_over_time(projected, squares, decay_offset, state, out_gain):
    seq_rows, local_heads = state.shape[:2]
    key_cols = local_heads * HEAD_KEY
    value_cols = local_heads * VALUE_CHANNELS
    projected = projected * lax.rsqrt(squares / D + epsilon)[:, None]
    value_rows = projected[:, :value_cols].reshape(seq_rows, local_heads, VALUE_CHANNELS)
    gate_rows = projected[:, value_cols : 2 * value_cols].reshape(
        seq_rows, local_heads, VALUE_CHANNELS
    )
    rest = projected[:, 2 * value_cols :]
    query_rows = rest[:, :key_cols].reshape(seq_rows, local_heads, HEAD_KEY)
    key_rows = rest[:, key_cols : 2 * key_cols].reshape(
        seq_rows, local_heads, HEAD_KEY
    ) * HEAD_KEY ** (-0.5)
    decay_logits = rest[:, 2 * key_cols : 3 * key_cols]
    decay_logarithm = jax.nn.log_sigmoid(decay_logits) / softness_factor + decay_offset
    decay_rate = jnp.exp(decay_logarithm).reshape(seq_rows, local_heads, HEAD_KEY)
    fresh = (
        decay_rate[:, :, :, None] * state + key_rows[:, :, :, None] * value_rows[:, :, None, :]
    )
    readout = jnp.sum(query_rows[:, :, :, None] * fresh, axis=2)
    normed = readout * lax.rsqrt(jnp.mean(readout * readout, axis=2, keepdims=True) + epsilon)
    normed = normed * out_gain.reshape(local_heads, VALUE_CHANNELS)[None]
    gated_out = (normed * jax.nn.silu(gate_rows)).reshape(seq_rows, value_cols)
    return gated_out.astype(jnp.bfloat16), fresh


def per_device(
    hidden_in,
    input_norm_gain,
    w_query,
    w_key,
    w_decay,
    w_value,
    w_gate,
    out_gain,
    w_out,
    decay_offset,
    state,
):
    seq_rows = state.shape[1]
    value_cols = w_out.shape[1]
    own_rows, features = hidden_in.shape
    n_dp, n_near = size_of(DP), size_of("near")
    matrices = (w_value, w_gate, w_query, w_key, w_decay)

    with jax.named_scope("gather_hidden"):
        hidden = copies(hidden_in, TP).reshape(-1, features)
    with jax.named_scope("fetch_out"):
        out_first = from_all(w_out[0])

    widened = hidden.astype(jnp.float32)
    scaled = (widened * input_norm_gain[0][None, :]).astype(jnp.bfloat16)
    partial_value = [dot(scaled, matrix[0]).astype(jnp.bfloat16) for matrix in matrices]
    used = sum(part.shape[1] for part in partial_value)
    sent = jnp.concatenate([hidden, *partial_value], axis=1)
    with jax.named_scope("sum_partials"):
        arrived = exchange(sent.reshape(n_dp, seq_rows, -1), DP)
    own = arrived[:, :, :features].astype(jnp.float32)
    gated_out, fresh_first = mixed_over_time(
        summed(arrived[:, :, features:]),
        jnp.sum(own * own, axis=(0, 2)),
        decay_offset[0],
        state[0],
        out_gain[0],
    )

    with jax.named_scope("fetch_in"):
        weights, arrived = lax.optimization_barrier(
            ([matrix[1] for matrix in matrices] + [w_out[1], input_norm_gain[1]], arrived)
        )
        rows = jnp.concatenate(
            [
                *(matrix.T for matrix in weights[:-2]),
                weights[-2],
                jnp.stack(three_terms(weights[-1])),
                jnp.zeros((13, features), jnp.bfloat16),
            ],
            axis=0,
        )
        fetched = from_all(rows)

    def out_terms(gated_out, pieces):
        return jnp.stack(
            [jnp.stack([dot(gated_out, part[i]) for i in range(part.shape[0])]) for part in pieces]
        ).astype(jnp.bfloat16)

    head_terms = turned_back(out_terms(gated_out, out_first))
    with jax.named_scope("near_sum"):
        near_sum = summed(exchange(head_terms.reshape(n_near, -1, seq_rows, features), "near"))
    with jax.named_scope("far_sum"):
        far_sum = summed(copies(near_sum.astype(jnp.bfloat16), "far"))
    before = lax.dynamic_index_in_dim(
        own.reshape(n_near, -1, seq_rows, features), lax.axis_index("near"), 0, keepdims=False
    )
    after = (before + far_sum).astype(jnp.bfloat16)
    with jax.named_scope("near_gather"):
        hidden = copies(after, "near").reshape(n_dp, seq_rows, features)

    widened = hidden.astype(jnp.float32)
    projected = 0.0
    for block, part in zip(turned(hidden), fetched):
        gain = summed(jnp.moveaxis(part[:, used + value_cols : used + value_cols + 3], 1, 0))
        scaled = (block.astype(jnp.float32) * gain[:, None, :]).astype(jnp.bfloat16)
        projected = projected + lax.dot_general(
            scaled,
            part[:, :used],
            (((0, 2), (0, 2)), ((), ())),
            preferred_element_type=jnp.float32,
        )
    gated_out, fresh_second = mixed_over_time(
        projected, jnp.sum(widened * widened, axis=(0, 2)), decay_offset[1], state[1], out_gain[1]
    )
    head_terms = turned_back(
        out_terms(gated_out, [part[:, used : used + value_cols] for part in fetched])
    )

    def to_holders(value):
        value = value.reshape(n_dp, n_near, own_rows, features)
        return jnp.moveaxis(value, 1, 0).reshape(n_near * n_dp, own_rows, features)

    with jax.named_scope("local_sum"):
        sent = jnp.concatenate(
            [to_holders(head_terms), to_holders(hidden)], axis=1
        )
        arrived = exchange(sent, LOCAL).reshape(n_near, n_dp, 2 * own_rows, features)
    before = lax.dynamic_index_in_dim(
        arrived[0], lax.axis_index("far"), 0, keepdims=False
    )[own_rows:]
    local_sum = summed(arrived[:, :, :own_rows])
    with jax.named_scope("far_scatter"):
        mixed = summed(exchange(local_sum.astype(jnp.bfloat16), "far"))
    hidden_out = (before.astype(jnp.float32) + mixed).astype(jnp.bfloat16)
    return (hidden_out, jnp.stack([fresh_first, fresh_second]))


def solution(mesh):
    sizes = mesh.shape
    fine = Mesh(
        mesh.devices.reshape(sizes["grp"], sizes["tp"] // NEAR, NEAR, sizes["dp"] // CORES, CORES),
        ("grp", *TP, *DP),
    )
    return jax.shard_map(
        per_device,
        mesh=fine,
        in_specs=(
            P(("grp", *TP), DP),
            P(None, DP),
            P(None, DP, TP),
            P(None, DP, TP),
            P(None, DP, TP),
            P(None, DP, TP),
            P(None, DP, TP),
            P(None, TP),
            P(None, TP, DP),
            P(None, ("grp", *DP), TP),
            P(None, ("grp", *DP), TP, None, None),
        ),
        out_specs=(P(("grp", *TP), DP), P(None, ("grp", *DP), TP, None, None)),
        check_vma=False,
    )
```

```python
import jax
import jax.numpy as jnp
from jax import lax
from jax.sharding import Mesh, PartitionSpec as P


D = 4096
HEAD_KEY = 64
VALUE_CHANNELS = 128
NEAR = 4
CORES = 2


epsilon = 1e-06
softness_factor = 16.0

TP = ("far", "near")
DP = ("x", "core")


def size_of(axes):
    return lax.psum(1, axes)


def exchange(blocks, axes):
    return lax.all_to_all(blocks, axes, split_axis=0, concat_axis=0, tiled=True)


def copies(value, axes):
    return exchange(jnp.broadcast_to(value[None], (size_of(axes), *value.shape)), axes)


def summed(blocks):
    return blocks.astype(jnp.float32).sum(axis=0)


def dot(left, right):
    return jnp.dot(left, right, preferred_element_type=jnp.float32)


def from_ring(value, held_for):
    n = size_of("x")
    onward = [(i, (i + 1) % n) for i in range(n)]
    back = [(i, (i - 1) % n) for i in range(n)]
    half = value.shape[0] // 2
    found = {0: value}
    ahead = behind = value
    for step in range(1, n // 2):
        found[step] = ahead = lax.ppermute(ahead, "x", onward)
        found[n - step] = behind = lax.ppermute(behind, "x", back)
    if held_for is not None:
        (ahead, behind), held_for = lax.optimization_barrier(((ahead, behind), held_for))
    found[n // 2] = jnp.concatenate(
        [lax.ppermute(ahead[:half], "x", onward), lax.ppermute(behind[half:], "x", back)],
        axis=0,
    )
    return jnp.stack([found[i] for i in range(n)]), held_for


def from_all(value, held_for=None):
    ours, held_for = from_ring(value, held_for)
    theirs = lax.ppermute(ours, "core", [(0, 1), (1, 0)])
    return (ours, theirs), held_for


def own_core_first(blocks, axis):
    return jnp.where(lax.axis_index("core") == 0, blocks, jnp.flip(blocks, axis))


def three_terms(value):
    terms = []
    for _ in range(3):
        term = lax.reduce_precision(value, 8, 7)
        terms.append(term.astype(jnp.bfloat16))
        value = value - term
    return terms


def mixed_over_time(projected, squares, decay_offset, state, out_gain):
    seq_rows, local_heads = state.shape[:2]
    key_cols = local_heads * HEAD_KEY
    value_cols = local_heads * VALUE_CHANNELS
    projected = projected * lax.rsqrt(squares / D + epsilon)[:, None]
    value_rows = projected[:, :value_cols].reshape(seq_rows, local_heads, VALUE_CHANNELS)
    gate_rows = projected[:, value_cols : 2 * value_cols].reshape(
        seq_rows, local_heads, VALUE_CHANNELS
    )
    rest = projected[:, 2 * value_cols :]
    query_rows = rest[:, :key_cols].reshape(seq_rows, local_heads, HEAD_KEY)
    key_rows = rest[:, key_cols : 2 * key_cols].reshape(
        seq_rows, local_heads, HEAD_KEY
    ) * HEAD_KEY ** (-0.5)
    decay_logits = rest[:, 2 * key_cols : 3 * key_cols]
    decay_logarithm = jax.nn.log_sigmoid(decay_logits) / softness_factor + decay_offset
    decay_rate = jnp.exp(decay_logarithm).reshape(seq_rows, local_heads, HEAD_KEY)
    fresh = (
        decay_rate[:, :, :, None] * state + key_rows[:, :, :, None] * value_rows[:, :, None, :]
    )
    readout = jnp.sum(query_rows[:, :, :, None] * fresh, axis=2)
    normed = readout * lax.rsqrt(jnp.mean(readout * readout, axis=2, keepdims=True) + epsilon)
    normed = normed * out_gain.reshape(local_heads, VALUE_CHANNELS)[None]
    gated_out = (normed * jax.nn.silu(gate_rows)).reshape(seq_rows, value_cols)
    return gated_out.astype(jnp.bfloat16), fresh


def per_device(
    hidden_in,
    input_norm_gain,
    w_query,
    w_key,
    w_decay,
    w_value,
    w_gate,
    out_gain,
    w_out,
    decay_offset,
    state,
):
    seq_rows = state.shape[1]
    value_cols = w_out.shape[1]
    own_rows, features = hidden_in.shape
    n_dp = size_of(DP)
    matrices = (w_value, w_gate, w_query, w_key, w_decay)

    hidden = copies(hidden_in, TP).reshape(-1, features)
    out_first, _ = from_all(w_out[0])
    rows = jnp.concatenate(
        [
            *(matrix[1].T for matrix in matrices),
            jnp.stack(three_terms(input_norm_gain[1])),
            jnp.zeros((13, features), jnp.bfloat16),
        ],
        axis=0,
    )

    widened = hidden.astype(jnp.float32)
    scaled = (widened * input_norm_gain[0][None, :]).astype(jnp.bfloat16)
    partial_value = [dot(scaled, matrix[0]).astype(jnp.bfloat16) for matrix in matrices]
    used = sum(part.shape[1] for part in partial_value)
    sent = jnp.concatenate([hidden, *partial_value], axis=1)
    arrived = exchange(sent.reshape(n_dp, seq_rows, -1), DP)
    fetched, arrived = from_all(rows, arrived)
    before = arrived[:, :, :features]
    own = before.astype(jnp.float32)
    gated_out, fresh_first = mixed_over_time(
        summed(arrived[:, :, features:]),
        jnp.sum(own * own, axis=(0, 2)),
        decay_offset[0],
        state[0],
        out_gain[0],
    )

    n_x = size_of("x")
    place, near = lax.axis_index("x"), lax.axis_index("near")
    head_terms = jnp.stack(
        [jnp.stack([dot(gated_out, part[i]) for part in out_first]) for i in range(n_x)]
    ).astype(jnp.bfloat16)
    near_sum = summed(exchange(head_terms, "near"))
    far_sum = summed(copies(near_sum.astype(jnp.bfloat16), "far"))
    before = lax.dynamic_index_in_dim(
        before.reshape(n_x, -1, seq_rows, features),
        lax.rem(place - near + n_x, n_x),
        0,
        keepdims=False,
    )
    after = own_core_first(before, 0).astype(jnp.float32) + far_sum
    hidden = copies(after.astype(jnp.bfloat16), "near")

    widened = hidden.astype(jnp.float32)
    projected = 0.0
    for i, part in enumerate(fetched):
        gain = summed(jnp.moveaxis(part[:, used : used + 3], 1, 0))
        scaled = (widened[:, i] * gain[:, None, :]).astype(jnp.bfloat16)
        projected = projected + lax.dot_general(
            scaled,
            part[:, :used],
            (((0, 2), (0, 2)), ((), ())),
            preferred_element_type=jnp.float32,
        )
    gated_out, fresh_second = mixed_over_time(
        projected,
        jnp.sum(widened * widened, axis=(0, 1, 3)),
        decay_offset[1],
        state[1],
        out_gain[1],
    )
    kept = lax.dynamic_slice_in_dim(hidden, near * own_rows, own_rows, 2)
    kept = own_core_first(kept, 1)
    kept = jnp.concatenate(
        [
            lax.dynamic_index_in_dim(kept, lax.rem(place - i + n_x, n_x), 0, keepdims=False)
            for i in range(n_x)
        ]
    ).reshape(n_dp, -1, value_cols)
    sent = jnp.concatenate(
        [jnp.broadcast_to(gated_out[None], (n_dp, *gated_out.shape)), kept], axis=1
    )
    arrived = exchange(sent, DP)
    head_terms = dot(arrived[:, :seq_rows].reshape(-1, value_cols), w_out[1])
    mixed = summed(exchange(head_terms.astype(jnp.bfloat16).reshape(-1, own_rows, features), TP))
    before = lax.dynamic_index_in_dim(
        arrived[:, seq_rows:], lax.axis_index("far"), 0, keepdims=False
    ).reshape(own_rows, features)
    hidden_out = (before.astype(jnp.float32) + mixed).astype(jnp.bfloat16)
    return (hidden_out, jnp.stack([fresh_first, fresh_second]))


def solution(mesh):
    sizes = mesh.shape
    fine = Mesh(
        mesh.devices.reshape(sizes["grp"], sizes["tp"] // NEAR, NEAR, sizes["dp"] // CORES, CORES),
        ("grp", *TP, *DP),
    )

    return jax.shard_map(
        per_device,
        mesh=fine,
        in_specs=(
            P(("grp", *TP), DP),
            P(None, DP),
            P(None, DP, TP),
            P(None, DP, TP),
            P(None, DP, TP),
            P(None, DP, TP),
            P(None, DP, TP),
            P(None, TP),
            P(None, TP, DP),
            P(None, ("grp", *DP), TP),
            P(None, ("grp", *DP), TP, None, None),
        ),
        out_specs=(P(("grp", *TP), DP), P(None, ("grp", *DP), TP, None, None)),
        check_vma=False,
    )
```

```python
import jax
import jax.numpy as jnp
from jax import lax
from jax.sharding import Mesh, PartitionSpec as P


D = 4096
HEAD_KEY = 64
VALUE_CHANNELS = 128
NEAR = 4
CORES = 2


epsilon = 1e-06
softness_factor = 16.0

TP = ("far", "near")
DP = ("x", "core")


def size_of(axes):
    return lax.psum(1, axes)


def exchange(blocks, axes):
    return lax.all_to_all(blocks, axes, split_axis=0, concat_axis=0, tiled=True)


def copies(value, axes):
    return exchange(jnp.broadcast_to(value[None], (size_of(axes), *value.shape)), axes)


def summed(blocks):
    return blocks.astype(jnp.float32).sum(axis=0)


def dot(left, right):
    return jnp.dot(left, right, preferred_element_type=jnp.float32)


def from_ring(value):
    n = size_of("x")
    half = value.shape[0] // 2

    def onward(part):
        return lax.ppermute(part, "x", [(i, (i + 1) % n) for i in range(n)])

    def back(part):
        return lax.ppermute(part, "x", [(i, (i - 1) % n) for i in range(n)])

    found = {0: value}
    ahead = behind = value
    for step in range(1, n // 2):
        found[step] = ahead = onward(ahead)
        found[n - step] = behind = back(behind)
    found[n // 2] = jnp.concatenate([onward(ahead[:half]), back(behind[half:])], axis=0)
    return jnp.stack([found[i] for i in range(n)])


def from_all(value):
    ours = from_ring(value)
    theirs = lax.ppermute(ours, "core", [(0, 1), (1, 0)])
    return ours, theirs


def own_core_first(blocks, axis):
    return jnp.where(lax.axis_index("core") == 0, blocks, jnp.flip(blocks, axis))


def three_terms(value):
    terms = []
    for _ in range(3):
        term = lax.reduce_precision(value, 8, 7)
        terms.append(term.astype(jnp.bfloat16))
        value = value - term
    return terms


def mixed_over_time(projected, squares, decay_offset, state, out_gain):
    seq_rows, local_heads = state.shape[:2]
    key_cols = local_heads * HEAD_KEY
    value_cols = local_heads * VALUE_CHANNELS
    projected = projected * lax.rsqrt(squares / D + epsilon)[:, None]
    value_rows = projected[:, :value_cols].reshape(seq_rows, local_heads, VALUE_CHANNELS)
    gate_rows = projected[:, value_cols : 2 * value_cols].reshape(
        seq_rows, local_heads, VALUE_CHANNELS
    )
    rest = projected[:, 2 * value_cols :]
    query_rows = rest[:, :key_cols].reshape(seq_rows, local_heads, HEAD_KEY)
    key_rows = rest[:, key_cols : 2 * key_cols].reshape(
        seq_rows, local_heads, HEAD_KEY
    ) * HEAD_KEY ** (-0.5)
    decay_logits = rest[:, 2 * key_cols : 3 * key_cols]
    decay_logarithm = jax.nn.log_sigmoid(decay_logits) / softness_factor + decay_offset
    decay_rate = jnp.exp(decay_logarithm).reshape(seq_rows, local_heads, HEAD_KEY)
    fresh = (
        decay_rate[:, :, :, None] * state + key_rows[:, :, :, None] * value_rows[:, :, None, :]
    )
    readout = jnp.sum(query_rows[:, :, :, None] * fresh, axis=2)
    normed = readout * lax.rsqrt(jnp.mean(readout * readout, axis=2, keepdims=True) + epsilon)
    normed = normed * out_gain.reshape(local_heads, VALUE_CHANNELS)[None]
    gated_out = (normed * jax.nn.silu(gate_rows)).reshape(seq_rows, value_cols)
    return gated_out.astype(jnp.bfloat16), fresh


def per_device(
    hidden_in,
    input_norm_gain,
    w_query,
    w_key,
    w_decay,
    w_value,
    w_gate,
    out_gain,
    w_out,
    decay_offset,
    state,
):
    seq_rows = state.shape[1]
    value_cols = w_out.shape[1]
    own_rows, features = hidden_in.shape
    n_dp = size_of(DP)
    matrices = (w_value, w_gate, w_query, w_key, w_decay)

    hidden = copies(hidden_in, TP).reshape(-1, features)
    out_first = from_all(w_out[0])
    widened = hidden.astype(jnp.float32)
    scaled = (widened * input_norm_gain[0][None, :]).astype(jnp.bfloat16)
    partial_value = [dot(scaled, matrix[0]).astype(jnp.bfloat16) for matrix in matrices]
    used = sum(part.shape[1] for part in partial_value)
    sent = jnp.concatenate([hidden, *partial_value], axis=1)
    arrived = exchange(sent.reshape(n_dp, seq_rows, -1), DP)
    weights, arrived = lax.optimization_barrier(
        ([matrix[1] for matrix in matrices] + [input_norm_gain[1]], arrived)
    )
    rows = jnp.concatenate(
        [
            *(matrix.T for matrix in weights[:-1]),
            jnp.stack(three_terms(weights[-1])),
            jnp.zeros((13, features), jnp.bfloat16),
        ],
        axis=0,
    )
    fetched = from_all(rows)
    before = arrived[:, :, :features]
    own = before.astype(jnp.float32)
    gated_out, fresh_first = mixed_over_time(
        summed(arrived[:, :, features:]),
        jnp.sum(own * own, axis=(0, 2)),
        decay_offset[0],
        state[0],
        out_gain[0],
    )

    n_x = size_of("x")
    place, near = lax.axis_index("x"), lax.axis_index("near")
    head_terms = jnp.stack(
        [jnp.stack([dot(gated_out, part[i]) for part in out_first]) for i in range(n_x)]
    ).astype(jnp.bfloat16)
    near_sum = summed(exchange(head_terms, "near"))
    far_sum = summed(copies(near_sum.astype(jnp.bfloat16), "far"))
    before = lax.dynamic_index_in_dim(
        before.reshape(n_x, -1, seq_rows, features),
        lax.rem(place - near + n_x, n_x),
        0,
        keepdims=False,
    )
    after = own_core_first(before, 0).astype(jnp.float32) + far_sum
    hidden = copies(after.astype(jnp.bfloat16), "near")

    widened = hidden.astype(jnp.float32)
    projected = 0.0
    for i, part in enumerate(fetched):
        gain = summed(jnp.moveaxis(part[:, used : used + 3], 1, 0))
        scaled = (widened[:, i] * gain[:, None, :]).astype(jnp.bfloat16)
        projected = projected + lax.dot_general(
            scaled,
            part[:, :used],
            (((0, 2), (0, 2)), ((), ())),
            preferred_element_type=jnp.float32,
        )
    gated_out, fresh_second = mixed_over_time(
        projected,
        jnp.sum(widened * widened, axis=(0, 1, 3)),
        decay_offset[1],
        state[1],
        out_gain[1],
    )
    kept = lax.dynamic_slice_in_dim(hidden, near * own_rows, own_rows, 2)
    kept = own_core_first(kept, 1)
    kept = jnp.concatenate(
        [
            lax.dynamic_index_in_dim(kept, lax.rem(place - i + n_x, n_x), 0, keepdims=False)
            for i in range(n_x)
        ]
    ).reshape(n_dp, -1, value_cols)
    sent = jnp.concatenate(
        [jnp.broadcast_to(gated_out[None], (n_dp, *gated_out.shape)), kept], axis=1
    )
    arrived = exchange(sent, DP)
    head_terms = dot(arrived[:, :seq_rows].reshape(-1, value_cols), w_out[1])
    mixed = summed(exchange(head_terms.astype(jnp.bfloat16).reshape(-1, own_rows, features), TP))
    before = lax.dynamic_index_in_dim(
        arrived[:, seq_rows:], lax.axis_index("far"), 0, keepdims=False
    ).reshape(own_rows, features)
    hidden_out = (before.astype(jnp.float32) + mixed).astype(jnp.bfloat16)
    return (hidden_out, jnp.stack([fresh_first, fresh_second]))


def solution(mesh):
    sizes = mesh.shape
    fine = Mesh(
        mesh.devices.reshape(sizes["grp"], sizes["tp"] // NEAR, NEAR, sizes["dp"] // CORES, CORES),
        ("grp", *TP, *DP),
    )

    return jax.shard_map(
        per_device,
        mesh=fine,
        in_specs=(
            P(("grp", *TP), DP),
            P(None, DP),
            P(None, DP, TP),
            P(None, DP, TP),
            P(None, DP, TP),
            P(None, DP, TP),
            P(None, DP, TP),
            P(None, TP),
            P(None, TP, DP),
            P(None, ("grp", *DP), TP),
            P(None, ("grp", *DP), TP, None, None),
        ),
        out_specs=(P(("grp", *TP), DP), P(None, ("grp", *DP), TP, None, None)),
        check_vma=False,
    )
```

```python
import jax
import jax.numpy as jnp
from jax import lax
from jax.sharding import Mesh, PartitionSpec as P


D = 4096
HEAD_KEY = 64
VALUE_CHANNELS = 128
LAYERS = 2
LANES = 128
NEAR = 4


epsilon = 1e-06
softness_factor = 16.0

TP = ("far", "near")


def size_of(axes):
    return lax.psum(1, axes)


def exchange(blocks, axes):
    return lax.all_to_all(blocks, axes, split_axis=0, concat_axis=0, tiled=True)


def copies(value, axes):
    return exchange(jnp.broadcast_to(value[None], (size_of(axes), *value.shape)), axes)


def summed(blocks):
    return blocks.astype(jnp.float32).sum(axis=0)


def two_terms(value):
    high = lax.reduce_precision(value, 8, 7)
    return high.astype(jnp.bfloat16), (value - high).astype(jnp.bfloat16)


def per_device(
    hidden_in,
    input_norm_gain,
    w_query,
    w_key,
    w_decay,
    w_value,
    w_gate,
    out_gain,
    w_out,
    decay_offset,
    state,
):
    seq_rows = state.shape[1]
    local_heads = state.shape[2]
    key_cols = local_heads * HEAD_KEY
    value_cols = local_heads * VALUE_CHANNELS
    own_rows, features = hidden_in.shape
    n_dp = size_of("dp")
    n_near = size_of("near")
    hidden = lax.optimization_barrier(copies(hidden_in, TP).reshape(-1, features))
    joined = lax.optimization_barrier(
        [
            jnp.concatenate(
                [m[i] for m in (w_value, w_gate, w_query, w_key, w_decay)], axis=1
            )
            for i in range(LAYERS)
        ]
    )
    gains, offsets = lax.optimization_barrier(
        (
            [out_gain[i].reshape(1, local_heads, VALUE_CHANNELS) for i in range(LAYERS)],
            [decay_offset[i] for i in range(LAYERS)],
        )
    )
    batch = hidden.shape[0]
    states = []
    for index_of_block in range(LAYERS):
        widened = hidden.astype(jnp.float32)
        squares = jnp.sum(widened * widened, axis=1, keepdims=True)
        scaled = (widened * input_norm_gain[index_of_block][None, :]).astype(jnp.bfloat16)
        partial_value = jnp.dot(
            scaled, joined[index_of_block], preferred_element_type=jnp.float32
        ).astype(jnp.bfloat16)
        used = partial_value.shape[1]
        spare = -(used + 2) % LANES
        sent = jnp.concatenate(
            [partial_value, *two_terms(squares), jnp.zeros((batch, spare), jnp.bfloat16)], axis=1
        )
        summed_parts = summed(exchange(sent.reshape(n_dp, seq_rows, -1), "dp"))
        own_squares = jnp.sum(summed_parts[:, used : used + 2], axis=1, keepdims=True)
        inverse = lax.rsqrt(own_squares / D + epsilon)
        projected = summed_parts[:, :used] * inverse
        value_rows = projected[:, :value_cols].reshape(seq_rows, local_heads, VALUE_CHANNELS)
        gate_rows = projected[:, value_cols : 2 * value_cols].reshape(
            seq_rows, local_heads, VALUE_CHANNELS
        )
        rest = projected[:, 2 * value_cols :]
        query_rows = rest[:, :key_cols].reshape(seq_rows, local_heads, HEAD_KEY)
        key_rows = rest[:, key_cols : 2 * key_cols].reshape(
            seq_rows, local_heads, HEAD_KEY
        ) * HEAD_KEY ** (-0.5)
        decay_logits = rest[:, 2 * key_cols :]
        decay_logarithm = (
            jax.nn.log_sigmoid(decay_logits) / softness_factor + offsets[index_of_block]
        )
        decay_rate = jnp.exp(decay_logarithm).reshape(seq_rows, local_heads, HEAD_KEY)
        fresh = (
            decay_rate[:, :, :, None] * state[index_of_block]
            + key_rows[:, :, :, None] * value_rows[:, :, None, :]
        )
        states.append(fresh)
        readout = jnp.sum(query_rows[:, :, :, None] * fresh, axis=2)
        normed = readout * lax.rsqrt(jnp.mean(readout * readout, axis=2, keepdims=True) + epsilon)
        normed = normed * gains[index_of_block]
        gated_out = (
            (normed * jax.nn.silu(gate_rows)).reshape(seq_rows, value_cols).astype(jnp.bfloat16)
        )
        head_terms = jnp.dot(
            copies(gated_out, "dp").reshape(batch, value_cols),
            w_out[index_of_block],
            preferred_element_type=jnp.float32,
        )
        head_terms = head_terms + hidden.astype(jnp.float32) * (1.0 / size_of(TP))
        head_terms = head_terms.astype(jnp.bfloat16)
        if index_of_block + 1 == LAYERS:
            blocks = head_terms.reshape(-1, n_near, own_rows, features).swapaxes(0, 1)
            near_sum = summed(exchange(blocks, "near"))
            hidden_out = summed(exchange(near_sum.astype(jnp.bfloat16), "far"))
        else:
            near_sum = summed(exchange(head_terms.reshape(n_near, -1, features), "near"))
            far_sum = summed(copies(near_sum.astype(jnp.bfloat16), "far"))
            hidden = copies(far_sum.astype(jnp.bfloat16), "near").reshape(batch, features)
    return (hidden_out.astype(jnp.bfloat16), jnp.stack(states))


def solution(mesh):
    sizes = mesh.shape
    fine = Mesh(
        mesh.devices.reshape(sizes["grp"], sizes["tp"] // NEAR, NEAR, sizes["dp"]),
        ("grp", *TP, "dp"),
    )

    return jax.shard_map(
        per_device,
        mesh=fine,
        in_specs=(
            P(("grp", *TP), "dp"),
            P(None, "dp"),
            P(None, "dp", TP),
            P(None, "dp", TP),
            P(None, "dp", TP),
            P(None, "dp", TP),
            P(None, "dp", TP),
            P(None, TP),
            P(None, TP, "dp"),
            P(None, ("grp", "dp"), TP),
            P(None, ("grp", "dp"), TP, None, None),
        ),
        out_specs=(P(("grp", *TP), "dp"), P(None, ("grp", "dp"), TP, None, None)),
        check_vma=False,
    )
```

```python
import jax
import jax.numpy as jnp
from jax import lax
from jax.sharding import Mesh, PartitionSpec as P


D = 4096
HEAD_KEY = 64
VALUE_CHANNELS = 128
LAYERS = 2
LANES = 128
NEAR = 4


epsilon = 1e-06
softness_factor = 16.0

HALVES = 2

TP = ("half", "stride", "near")
FAR = ("stride", "half")


def size_of(axes):
    return lax.psum(1, axes)


def exchange(blocks, axes):
    return lax.all_to_all(blocks, axes, split_axis=0, concat_axis=0, tiled=True)


def copies(value, axes):
    return exchange(jnp.broadcast_to(value[None], (size_of(axes), *value.shape)), axes)


def summed(blocks):
    return blocks.astype(jnp.float32).sum(axis=0)


def two_terms(value):
    high = lax.reduce_precision(value, 8, 7)
    return high.astype(jnp.bfloat16), (value - high).astype(jnp.bfloat16)


def per_device(
    hidden_in,
    input_norm_gain,
    w_query,
    w_key,
    w_decay,
    w_value,
    w_gate,
    out_gain,
    w_out,
    decay_offset,
    state,
):
    seq_rows = state.shape[1]
    local_heads = state.shape[2]
    key_cols = local_heads * HEAD_KEY
    value_cols = local_heads * VALUE_CHANNELS
    own_rows, features = hidden_in.shape
    n_dp = size_of("dp")
    n_near = size_of("near")
    hidden = lax.optimization_barrier(copies(hidden_in, TP).reshape(-1, features))
    joined = lax.optimization_barrier(
        [
            jnp.concatenate(
                [m[i] for m in (w_value, w_gate, w_query, w_key, w_decay)], axis=1
            )
            for i in range(LAYERS)
        ]
    )
    gains, offsets = lax.optimization_barrier(
        (
            [out_gain[i].reshape(1, local_heads, VALUE_CHANNELS) for i in range(LAYERS)],
            [decay_offset[i] for i in range(LAYERS)],
        )
    )
    batch = hidden.shape[0]
    states = []
    for index_of_block in range(LAYERS):
        widened = hidden.astype(jnp.float32)
        squares = jnp.sum(widened * widened, axis=1, keepdims=True)
        scaled = (widened * input_norm_gain[index_of_block][None, :]).astype(jnp.bfloat16)
        partial_value = jnp.dot(
            scaled, joined[index_of_block], preferred_element_type=jnp.float32
        ).astype(jnp.bfloat16)
        used = partial_value.shape[1]
        spare = -(used + 2) % LANES
        sent = jnp.concatenate(
            [partial_value, *two_terms(squares), jnp.zeros((batch, spare), jnp.bfloat16)], axis=1
        )
        summed_parts = summed(exchange(sent.reshape(n_dp, seq_rows, -1), "dp"))
        own_squares = jnp.sum(summed_parts[:, used : used + 2], axis=1, keepdims=True)
        inverse = lax.rsqrt(own_squares / D + epsilon)
        projected = summed_parts[:, :used] * inverse
        value_rows = projected[:, :value_cols].reshape(seq_rows, local_heads, VALUE_CHANNELS)
        gate_rows = projected[:, value_cols : 2 * value_cols].reshape(
            seq_rows, local_heads, VALUE_CHANNELS
        )
        rest = projected[:, 2 * value_cols :]
        query_rows = rest[:, :key_cols].reshape(seq_rows, local_heads, HEAD_KEY)
        key_rows = rest[:, key_cols : 2 * key_cols].reshape(
            seq_rows, local_heads, HEAD_KEY
        ) * HEAD_KEY ** (-0.5)
        decay_logits = rest[:, 2 * key_cols :]
        decay_logarithm = (
            jax.nn.log_sigmoid(decay_logits) / softness_factor + offsets[index_of_block]
        )
        decay_rate = jnp.exp(decay_logarithm).reshape(seq_rows, local_heads, HEAD_KEY)
        fresh = (
            decay_rate[:, :, :, None] * state[index_of_block]
            + key_rows[:, :, :, None] * value_rows[:, :, None, :]
        )
        states.append(fresh)
        readout = jnp.sum(query_rows[:, :, :, None] * fresh, axis=2)
        normed = readout * lax.rsqrt(jnp.mean(readout * readout, axis=2, keepdims=True) + epsilon)
        normed = normed * gains[index_of_block]
        gated_out = (
            (normed * jax.nn.silu(gate_rows)).reshape(seq_rows, value_cols).astype(jnp.bfloat16)
        )
        head_terms = jnp.dot(
            copies(gated_out, "dp").reshape(batch, value_cols),
            w_out[index_of_block],
            preferred_element_type=jnp.float32,
        )
        head_terms = head_terms + hidden.astype(jnp.float32) * (1.0 / size_of(TP))
        head_terms = head_terms.astype(jnp.bfloat16)
        if index_of_block + 1 == LAYERS:
            blocks = head_terms.reshape(HALVES, -1, n_near, own_rows, features)
            blocks = blocks.transpose(2, 1, 0, 3, 4).reshape(n_near, -1, own_rows, features)
            near_sum = summed(exchange(blocks, "near"))
            hidden_out = summed(exchange(near_sum.astype(jnp.bfloat16), FAR))
        else:
            near_sum = summed(exchange(head_terms.reshape(n_near, -1, features), "near"))
            far_sum = summed(copies(near_sum.astype(jnp.bfloat16), FAR))
            hidden = copies(far_sum.astype(jnp.bfloat16), "near").reshape(batch, features)
    return (hidden_out.astype(jnp.bfloat16), jnp.stack(states))


def solution(mesh):
    sizes = mesh.shape
    fine = Mesh(
        mesh.devices.reshape(
            sizes["grp"], HALVES, sizes["tp"] // (HALVES * NEAR), NEAR, sizes["dp"]
        ),
        ("grp", *TP, "dp"),
    )

    return jax.shard_map(
        per_device,
        mesh=fine,
        in_specs=(
            P(("grp", *TP), "dp"),
            P(None, "dp"),
            P(None, "dp", TP),
            P(None, "dp", TP),
            P(None, "dp", TP),
            P(None, "dp", TP),
            P(None, "dp", TP),
            P(None, TP),
            P(None, TP, "dp"),
            P(None, ("grp", "dp"), TP),
            P(None, ("grp", "dp"), TP, None, None),
        ),
        out_specs=(P(("grp", *TP), "dp"), P(None, ("grp", "dp"), TP, None, None)),
        check_vma=False,
    )
```

```python
import jax
import jax.numpy as jnp
from jax import lax
from jax.sharding import Mesh, PartitionSpec as P


D = 4096
HEAD_KEY = 64
VALUE_CHANNELS = 128
LAYERS = 2
LANES = 128
NEAR = 4


epsilon = 1e-06
softness_factor = 16.0

HALVES = 2

TP = ("half", "quarter", "eighth", "near")
FAR = ("quarter", "eighth", "half")


def size_of(axes):
    return lax.psum(1, axes)


def exchange(blocks, axes):
    return lax.all_to_all(blocks, axes, split_axis=0, concat_axis=0, tiled=True)


def copies(value, axes):
    return exchange(jnp.broadcast_to(value[None], (size_of(axes), *value.shape)), axes)


def summed(blocks):
    return blocks.astype(jnp.float32).sum(axis=0)


def two_terms(value):
    high = lax.reduce_precision(value, 8, 7)
    return high.astype(jnp.bfloat16), (value - high).astype(jnp.bfloat16)


def per_device(
    hidden_in,
    input_norm_gain,
    w_query,
    w_key,
    w_decay,
    w_value,
    w_gate,
    out_gain,
    w_out,
    decay_offset,
    state,
):
    seq_rows = state.shape[1]
    local_heads = state.shape[2]
    key_cols = local_heads * HEAD_KEY
    value_cols = local_heads * VALUE_CHANNELS
    own_rows, features = hidden_in.shape
    n_dp = size_of("dp")
    n_near = size_of("near")
    hidden = lax.optimization_barrier(copies(hidden_in, TP).reshape(-1, features))
    joined = lax.optimization_barrier(
        [
            jnp.concatenate(
                [m[i] for m in (w_value, w_gate, w_query, w_key, w_decay)], axis=1
            )
            for i in range(LAYERS)
        ]
    )
    gains, offsets = lax.optimization_barrier(
        (
            [out_gain[i].reshape(1, local_heads, VALUE_CHANNELS) for i in range(LAYERS)],
            [decay_offset[i] for i in range(LAYERS)],
        )
    )
    batch = hidden.shape[0]
    states = []
    for index_of_block in range(LAYERS):
        widened = hidden.astype(jnp.float32)
        squares = jnp.sum(widened * widened, axis=1, keepdims=True)
        scaled = (widened * input_norm_gain[index_of_block][None, :]).astype(jnp.bfloat16)
        partial_value = jnp.dot(
            scaled, joined[index_of_block], preferred_element_type=jnp.float32
        ).astype(jnp.bfloat16)
        used = partial_value.shape[1]
        spare = -(used + 2) % LANES
        sent = jnp.concatenate(
            [partial_value, *two_terms(squares), jnp.zeros((batch, spare), jnp.bfloat16)], axis=1
        )
        summed_parts = summed(exchange(sent.reshape(n_dp, seq_rows, -1), "dp"))
        own_squares = jnp.sum(summed_parts[:, used : used + 2], axis=1, keepdims=True)
        inverse = lax.rsqrt(own_squares / D + epsilon)
        projected = summed_parts[:, :used] * inverse
        value_rows = projected[:, :value_cols].reshape(seq_rows, local_heads, VALUE_CHANNELS)
        gate_rows = projected[:, value_cols : 2 * value_cols].reshape(
            seq_rows, local_heads, VALUE_CHANNELS
        )
        rest = projected[:, 2 * value_cols :]
        query_rows = rest[:, :key_cols].reshape(seq_rows, local_heads, HEAD_KEY)
        key_rows = rest[:, key_cols : 2 * key_cols].reshape(
            seq_rows, local_heads, HEAD_KEY
        ) * HEAD_KEY ** (-0.5)
        decay_logits = rest[:, 2 * key_cols :]
        decay_logarithm = (
            jax.nn.log_sigmoid(decay_logits) / softness_factor + offsets[index_of_block]
        )
        decay_rate = jnp.exp(decay_logarithm).reshape(seq_rows, local_heads, HEAD_KEY)
        fresh = (
            decay_rate[:, :, :, None] * state[index_of_block]
            + key_rows[:, :, :, None] * value_rows[:, :, None, :]
        )
        states.append(fresh)
        readout = jnp.sum(query_rows[:, :, :, None] * fresh, axis=2)
        normed = readout * lax.rsqrt(jnp.mean(readout * readout, axis=2, keepdims=True) + epsilon)
        normed = normed * gains[index_of_block]
        gated_out = (
            (normed * jax.nn.silu(gate_rows)).reshape(seq_rows, value_cols).astype(jnp.bfloat16)
        )
        head_terms = jnp.dot(
            copies(gated_out, "dp").reshape(batch, value_cols),
            w_out[index_of_block],
            preferred_element_type=jnp.float32,
        )
        head_terms = head_terms + hidden.astype(jnp.float32) * (1.0 / size_of(TP))
        head_terms = head_terms.astype(jnp.bfloat16)
        if index_of_block + 1 == LAYERS:
            blocks = head_terms.reshape(HALVES, -1, n_near, own_rows, features)
            blocks = blocks.transpose(2, 1, 0, 3, 4).reshape(n_near, -1, own_rows, features)
            near_sum = summed(exchange(blocks, "near"))
            hidden_out = summed(exchange(near_sum.astype(jnp.bfloat16), FAR))
        else:
            wide = ("eighth", "near")
            near_sum = summed(exchange(head_terms.reshape(size_of(wide), -1, features), wide))
            far_sum = summed(copies(near_sum.astype(jnp.bfloat16), ("quarter", "half")))
            hidden = copies(far_sum.astype(jnp.bfloat16), wide).reshape(batch, features)
    return (hidden_out.astype(jnp.bfloat16), jnp.stack(states))


def solution(mesh):
    sizes = mesh.shape
    fine = Mesh(
        mesh.devices.reshape(
            sizes["grp"], HALVES, sizes["tp"] // (2 * HALVES * NEAR), 2, NEAR, sizes["dp"]
        ),
        ("grp", *TP, "dp"),
    )

    return jax.shard_map(
        per_device,
        mesh=fine,
        in_specs=(
            P(("grp", *TP), "dp"),
            P(None, "dp"),
            P(None, "dp", TP),
            P(None, "dp", TP),
            P(None, "dp", TP),
            P(None, "dp", TP),
            P(None, "dp", TP),
            P(None, TP),
            P(None, TP, "dp"),
            P(None, ("grp", "dp"), TP),
            P(None, ("grp", "dp"), TP, None, None),
        ),
        out_specs=(P(("grp", *TP), "dp"), P(None, ("grp", "dp"), TP, None, None)),
        check_vma=False,
    )
```

```python
import jax
import jax.numpy as jnp
from jax import lax
from jax.sharding import Mesh, PartitionSpec as P


D = 4096
HEAD_KEY = 64
VALUE_CHANNELS = 128
LAYERS = 2
LANES = 128
NEAR = 4


epsilon = 1e-06
softness_factor = 16.0

HALVES = 2

TP = ("half", "quarter", "eighth", "near")
FAR = ("quarter", "eighth", "half")


def size_of(axes):
    return lax.psum(1, axes)


def exchange(blocks, axes):
    return lax.all_to_all(blocks, axes, split_axis=0, concat_axis=0, tiled=True)


def copies(value, axes):
    return exchange(jnp.broadcast_to(value[None], (size_of(axes), *value.shape)), axes)


def summed(blocks):
    return blocks.astype(jnp.float32).sum(axis=0)


def two_terms(value):
    high = lax.reduce_precision(value, 8, 7)
    return high.astype(jnp.bfloat16), (value - high).astype(jnp.bfloat16)


def per_device(
    hidden_in,
    input_norm_gain,
    w_query,
    w_key,
    w_decay,
    w_value,
    w_gate,
    out_gain,
    w_out,
    decay_offset,
    state,
):
    seq_rows = state.shape[1]
    local_heads = state.shape[2]
    key_cols = local_heads * HEAD_KEY
    value_cols = local_heads * VALUE_CHANNELS
    own_rows, features = hidden_in.shape
    n_dp = size_of("dp")
    n_near = size_of("near")
    hidden = copies(hidden_in, ("half", "quarter", "eighth"))
    hidden = copies(hidden, "near").swapaxes(0, 1).reshape(-1, features)
    hidden = lax.optimization_barrier(hidden)
    joined = lax.optimization_barrier(
        [
            jnp.concatenate(
                [m[i] for m in (w_value, w_gate, w_query, w_key, w_decay)], axis=1
            )
            for i in range(LAYERS)
        ]
    )
    gains, offsets = lax.optimization_barrier(
        (
            [out_gain[i].reshape(1, local_heads, VALUE_CHANNELS) for i in range(LAYERS)],
            [decay_offset[i] for i in range(LAYERS)],
        )
    )
    batch = hidden.shape[0]
    states = []
    for index_of_block in range(LAYERS):
        widened = hidden.astype(jnp.float32)
        squares = jnp.sum(widened * widened, axis=1, keepdims=True)
        scaled = (widened * input_norm_gain[index_of_block][None, :]).astype(jnp.bfloat16)
        partial_value = jnp.dot(
            scaled, joined[index_of_block], preferred_element_type=jnp.float32
        ).astype(jnp.bfloat16)
        used = partial_value.shape[1]
        spare = -(used + 2) % LANES
        sent = jnp.concatenate(
            [partial_value, *two_terms(squares), jnp.zeros((batch, spare), jnp.bfloat16)], axis=1
        )
        summed_parts = summed(exchange(sent.reshape(n_dp, seq_rows, -1), "dp"))
        own_squares = jnp.sum(summed_parts[:, used : used + 2], axis=1, keepdims=True)
        inverse = lax.rsqrt(own_squares / D + epsilon)
        projected = summed_parts[:, :used] * inverse
        value_rows = projected[:, :value_cols].reshape(seq_rows, local_heads, VALUE_CHANNELS)
        gate_rows = projected[:, value_cols : 2 * value_cols].reshape(
            seq_rows, local_heads, VALUE_CHANNELS
        )
        rest = projected[:, 2 * value_cols :]
        query_rows = rest[:, :key_cols].reshape(seq_rows, local_heads, HEAD_KEY)
        key_rows = rest[:, key_cols : 2 * key_cols].reshape(
            seq_rows, local_heads, HEAD_KEY
        ) * HEAD_KEY ** (-0.5)
        decay_logits = rest[:, 2 * key_cols :]
        decay_logarithm = (
            jax.nn.log_sigmoid(decay_logits) / softness_factor + offsets[index_of_block]
        )
        decay_rate = jnp.exp(decay_logarithm).reshape(seq_rows, local_heads, HEAD_KEY)
        fresh = (
            decay_rate[:, :, :, None] * state[index_of_block]
            + key_rows[:, :, :, None] * value_rows[:, :, None, :]
        )
        states.append(fresh)
        readout = jnp.sum(query_rows[:, :, :, None] * fresh, axis=2)
        normed = readout * lax.rsqrt(jnp.mean(readout * readout, axis=2, keepdims=True) + epsilon)
        normed = normed * gains[index_of_block]
        gated_out = (
            (normed * jax.nn.silu(gate_rows)).reshape(seq_rows, value_cols).astype(jnp.bfloat16)
        )
        head_terms = jnp.dot(
            copies(gated_out, "dp").reshape(batch, value_cols),
            w_out[index_of_block],
            preferred_element_type=jnp.float32,
        )
        head_terms = head_terms + hidden.astype(jnp.float32) * (1.0 / size_of(TP))
        head_terms = head_terms.astype(jnp.bfloat16)
        if index_of_block + 1 == LAYERS:
            blocks = head_terms.reshape(HALVES, -1, n_near, own_rows, features)
            blocks = blocks.transpose(2, 1, 0, 3, 4).reshape(n_near, -1, own_rows, features)
            near_sum = summed(exchange(blocks, "near"))
            hidden_out = summed(exchange(near_sum.astype(jnp.bfloat16), FAR))
        else:
            near_sum = summed(exchange(head_terms.reshape(n_near, -1, features), "near"))
            far_sum = summed(copies(near_sum.astype(jnp.bfloat16), ("half", "eighth", "quarter")))
            hidden = copies(far_sum.astype(jnp.bfloat16), "near").reshape(batch, features)
    return (hidden_out.astype(jnp.bfloat16), jnp.stack(states))


def solution(mesh):
    sizes = mesh.shape
    fine = Mesh(
        mesh.devices.reshape(
            sizes["grp"], HALVES, sizes["tp"] // (2 * HALVES * NEAR), 2, NEAR, sizes["dp"]
        ),
        ("grp", *TP, "dp"),
    )

    return jax.shard_map(
        per_device,
        mesh=fine,
        in_specs=(
            P(("grp", *TP), "dp"),
            P(None, "dp"),
            P(None, "dp", TP),
            P(None, "dp", TP),
            P(None, "dp", TP),
            P(None, "dp", TP),
            P(None, "dp", TP),
            P(None, TP),
            P(None, TP, "dp"),
            P(None, ("grp", "dp"), TP),
            P(None, ("grp", "dp"), TP, None, None),
        ),
        out_specs=(P(("grp", *TP), "dp"), P(None, ("grp", "dp"), TP, None, None)),
        check_vma=False,
    )
```
